256 devices in a mesh: ep: 64 (over z, y, core), tp: 4 (over x).
Axes of the slice: x: 4, y: 4, z: 8, core: 2. Of those that a mesh axis runs over, the one named last changes fastest.
Arguments:
- query_rows: bfloat16 [8192, 1024], P('ep', 'tp'), may hold values from -10 to 10
- key_rows: bfloat16 [8192, 1024], P('ep', 'tp'), may hold values from -10 to 10
- value_rows: bfloat16 [8192, 1024], P('ep', 'tp'), may hold values from -6 to 6
- key_bias: bfloat16 [8192, 16], P('ep', 'tp'), may hold values from -24 to 4
- mixer_weight: bfloat16 [1024, 2048], P('tp'), may hold values from -0.1875 to 0.1875
- mixer_gain: float32 [2048], replicated, may hold values from 0.1 to 1.9
- routed_input: bfloat16 [24576, 2048], P(('ep', 'tp')), may hold values from -6 to 6
- entry_gain: float32 [2048], replicated, may hold values from 0.1 to 1.9
- expert_index: int32 [24576, 2], P(('ep', 'tp')), may hold values from 0 to 127, all different within a row; in each aligned block of 96 rows (0 to 95, 96 to 191, ...) at most 2 rows name the same one
- route_weights: float32 [24576, 2], P(('ep', 'tp')), may hold values from 0.1 to 1
- expert_gate: bfloat16 [128, 2048, 1024], P('ep', None, 'tp'), may hold values from -0.125 to 0.125
- expert_up: bfloat16 [128, 2048, 1024], P('ep', None, 'tp'), may hold values from -0.125 to 0.125
- expert_down: bfloat16 [128, 1024, 2048], P('ep', 'tp'), may hold values from -0.1875 to 0.1875
- shared_gate: bfloat16 [2048, 1024], P(None, 'tp'), may hold values from -0.125 to 0.125
- shared_up: bfloat16 [2048, 1024], P(None, 'tp'), may hold values from -0.125 to 0.125
- shared_down: bfloat16 [1024, 2048], P('tp'), may hold values from -0.1875 to 0.1875
- exit_gain: float32 [2048], replicated, may hold values from 0.1 to 1.9
Outputs:
- mixer_out: bfloat16 [8192, 2048], P(('ep', 'tp'))
- expert_out: bfloat16 [24576, 2048], P(('ep', 'tp'))
The draws below stay inside these ranges and needn't reach their ends.
Inputs may be any that keep to these rules, and one draw needn't show every extreme that they name: `expert_index`: in each aligned block of 96 rows (the rows of one device) no expert is named by more than 2 rows, a bound that some block reaches; each row names 2 different experts.
All inputs are finite; a program needn't handle non-finite values.
Results may differ from the reference program's by a relative error of at most 0.012.
Values may be sent and summed in bfloat16 or wider, within the bound.
No kernel may reach another device: no remote copies, remote signals or barrier semaphores. Data moves between devices by JAX's collectives and lax.ppermute only.
A program may use at most 128 MiB of HBM per device.

```python
import math
import jax
import jax.numpy as jnp
import numpy as np
from jax import lax

D = 2048
HEADS = 16
HEAD_DIM = 64
FF = 1024
FF_SH = 1024
TOPK = 2
TOK_A = 128
ROWS_B = 96
TOKENS_A = 8192
TOKENS_B = 24576
EXPERTS = 128
CAP = 2
N_EP = 64
N_TP = 4


def draw_key_bias(key, part):
    random_subkeys = jax.random.split(key, 7)
    sequence_length = TOKENS_A
    head_count = HEADS
    head_draw = jax.random.uniform(random_subkeys[0], (head_count,))
    quick_heads = (head_draw < 0.5) | (head_draw <= jnp.min(head_draw))
    keep_share = jax.random.uniform(random_subkeys[1], (head_count,), minval=0.4, maxval=1.2)
    fast_reach = jax.random.uniform(random_subkeys[2], (head_count,), minval=30.0, maxval=50.0)
    noise_shift = 3.3
    slow_level = jnp.log(keep_share / sequence_length) - noise_shift
    fast_level = -jnp.log(fast_reach) - noise_shift
    base_level = jnp.where(quick_heads, fast_level, slow_level)
    shard_count = sequence_length // TOK_A
    shard_shift = jax.random.uniform(random_subkeys[3], (shard_count, head_count), minval=-0.7, maxval=0.7)
    shard_shift = jnp.repeat(shard_shift, TOK_A, axis=0)
    roughness = 0.3 * jax.random.normal(random_subkeys[4], (sequence_length, head_count))
    logarithm_bias = base_level[None, :] + shard_shift + roughness
    spike_positions = jax.random.randint(random_subkeys[5], (3,), 0, sequence_length)
    spike_rows = jnp.any(jnp.arange(sequence_length)[:, None] == spike_positions[None, :], axis=1)
    remaining_fraction = jax.random.uniform(random_subkeys[6], (sequence_length, head_count), minval=0.2, maxval=0.5)
    spike_level = jnp.log(remaining_fraction / (1.0 - remaining_fraction))
    logarithm_bias = jnp.where(spike_rows[:, None] & (~quick_heads)[None, :], spike_level, logarithm_bias)
    return logarithm_bias.astype(jnp.float32).astype(jnp.bfloat16)


def block_levels(key, dims, cuts, low, largest):
    level, own = 1.0, jax.random.fold_in(key, 6)
    for axis_at, blocks in cuts:
        heights = jnp.exp(jax.random.uniform(jax.random.fold_in(own, axis_at), (blocks,), jnp.float32, low / len(cuts), largest / len(cuts)))
        level = level * jnp.repeat(heights, dims[axis_at] // blocks).reshape([-1 if axis == axis_at else 1 for axis in range(len(dims))])
    return level


def deal_out(own_key, own, number, rows, number_of, top, reach, skew):
    ranking = jax.random.permutation(own_key, number_of)
    heavy_load, common = shares(number_of, rows * top, reach, skew, True), shares(number_of, rows * top, reach, skew, False)
    places = jnp.arange(number_of)

    def named(tallies, offset_by):
        used = int((tallies > 0).sum())
        fixed = max(1, used // 4)
        moved = fixed + (places - fixed + offset_by * (used - fixed)) % max(1, number_of - fixed)
        return jnp.zeros((number_of,), jnp.int32).at[ranking[jnp.where(places < fixed, places, moved)]].set(jnp.asarray(tallies, jnp.int32))

    tallies = jnp.where(number % 4 == 0, named(heavy_load, number // 4), named(common, number - number // 4 - 1))
    mixed = jax.random.permutation(jax.random.fold_in(own, 3), number_of)
    source_of, receiver = mixed[0:number_of // 2 * 2:2], mixed[1:number_of // 2 * 2:2]
    margin = jnp.minimum(tallies[source_of] - 1, reach - tallies[receiver]) // 2
    margin = jnp.where((source_of == ranking[0]) | (receiver == ranking[0]) | (tallies[receiver] == 0), 0, jnp.maximum(margin, 0))
    moved = jax.random.randint(jax.random.fold_in(own, 4), (number_of // 2,), 0, 1 << 20) % (margin + 1)
    tallies = tallies.at[source_of].add(-moved).at[receiver].add(moved)
    labels = jnp.searchsorted(jnp.cumsum(tallies), jnp.arange(rows * top), side="right").astype(jnp.int32)
    listing = labels.reshape(top, rows).T
    listing = listing[jax.random.permutation(jax.random.fold_in(own, 1), rows)]
    offset_by = jax.random.randint(jax.random.fold_in(own, 2), (rows, 1), 0, top)
    return jnp.take_along_axis(listing, (jnp.arange(top)[None, :] + offset_by) % top, axis=1)


def shares(count, total, bound, slope, full):
    loads = [(1 << 20) // math.isqrt(grade ** slope) + 1 for grade in range(1, count + 1)]
    largest = bound if full else min(bound, max(-(-total // count), total * loads[0] // sum(loads)))
    least = 1 if total - largest >= count - 1 else 0
    holding, surplus = [largest] + [least] * (count - 1), total - largest - least * (count - 1)
    while surplus > 0:
        movable = [i for i in range(1, count) if holding[i] < largest] or [i for i in range(1, count) if holding[i] < bound]
        whole, left = sum([loads[i] for i in movable]), surplus
        for i in movable:
            addition = min(bound - holding[i], max(1, left * loads[i] // whole), surplus)
            holding[i] = holding[i] + addition
            surplus = surplus - addition
    return np.array(holding)


def gaussian(rng, shape, deviation, bound, cuts=(), kind=jnp.bfloat16):
    array = jax.random.normal(rng, shape, jnp.float32) * deviation
    if len(cuts) > 0:
        array = block_levels(rng, shape, cuts, -0.22, 0.18) * array
    return jnp.clip(array, min=-bound, max=bound).astype(kind)


def setup_inputs(seed: int = 0) -> dict:
    seeds = jax.random.split(jax.random.key(seed), 18)
    query_rows = gaussian(seeds[0], (TOKENS_A, HEADS * HEAD_DIM), 1.6, 10.0, ((0, 64), (1, 4)))
    key_rows = gaussian(seeds[1], (TOKENS_A, HEADS * HEAD_DIM), 1.6, 10.0, ((0, 64), (1, 4)))
    value_rows = gaussian(seeds[2], (TOKENS_A, HEADS * HEAD_DIM), 1.0, 6.0, ((0, 64), (1, 4)))
    key_bias = draw_key_bias(jax.random.fold_in(seeds[17], 71), 0)
    mixer_weight = gaussian(seeds[4], (HEADS * HEAD_DIM, D), (HEADS * HEAD_DIM) ** -0.5, 0.1875, ((0, 4),))
    mixer_gain = jnp.clip(1.0 + 0.18 * jax.random.normal(seeds[5], (D,), jnp.float32), 0.1, 1.9)
    routed_input = gaussian(seeds[6], (TOKENS_B, D), 1.0, 6.0, ((0, 256),))
    entry_gain = jnp.clip(1.0 + 0.18 * jax.random.normal(seeds[7], (D,), jnp.float32), 0.1, 1.9)
    expert_index_keys = jax.random.split(jax.random.fold_in(seeds[8], 1), TOKENS_B // ROWS_B)
    expert_index_turns = jax.random.permutation(jax.random.fold_in(seeds[8], 3), TOKENS_B // ROWS_B)
    expert_index = jax.vmap(lambda own, number: deal_out(jax.random.fold_in(seeds[8], 2), own, number, ROWS_B, EXPERTS, TOPK, CAP, 2))(expert_index_keys, expert_index_turns).reshape((TOKENS_B, TOPK))
    route_weights = jnp.clip(jnp.exp(math.log(1.0) - 2.3025851 * jax.random.uniform(seeds[9], (TOKENS_B, TOPK), jnp.float32) ** block_levels(seeds[9], (TOKENS_B, TOPK), ((0, 256),), -0.2, 0.2)), 0.1, 1.0)
    expert_gate = gaussian(seeds[10], (EXPERTS, D, FF), D ** -0.5, 0.125, ((0, 64), (2, 4)))
    expert_up = gaussian(seeds[11], (EXPERTS, D, FF), D ** -0.5, 0.125, ((0, 64), (2, 4)))
    expert_down = gaussian(seeds[12], (EXPERTS, FF, D), FF ** -0.5, 0.1875, ((0, 64), (1, 4)))
    shared_gate = gaussian(seeds[13], (D, FF_SH), D ** -0.5, 0.125, ((1, 4),))
    shared_up = gaussian(seeds[14], (D, FF_SH), D ** -0.5, 0.125, ((1, 4),))
    shared_down = gaussian(seeds[15], (FF_SH, D), FF_SH ** -0.5, 0.1875, ((0, 4),))
    exit_gain = jnp.clip(1.0 + 0.18 * jax.random.normal(seeds[16], (D,), jnp.float32), 0.1, 1.9)
    return dict(query_rows=query_rows, key_rows=key_rows, value_rows=value_rows, key_bias=key_bias, mixer_weight=mixer_weight, mixer_gain=mixer_gain, routed_input=routed_input, entry_gain=entry_gain, expert_index=expert_index, route_weights=route_weights, expert_gate=expert_gate, expert_up=expert_up, expert_down=expert_down, shared_gate=shared_gate, shared_up=shared_up, shared_down=shared_down, exit_gain=exit_gain)


EPS = 1e-06

def root_norm(values, gain_row):
    return values * lax.rsqrt(lax.optimization_barrier(jnp.mean(values * values, axis=-1, keepdims=True)) + EPS) * gain_row

def key_shards():
    shards = 1
    while shards * TOK_A < 512 and N_EP % (2 * shards) == 0:
        shards = shards * 2
    return shards

def stick_breaking(query_rows, key_rows, value_rows, key_bias):
    total_rows = query_rows.shape[0]
    block_rows = key_shards() * TOK_A
    query_split = query_rows.reshape(N_EP, TOK_A, HEADS, HEAD_DIM).astype(jnp.float32)
    keys_split = key_rows.reshape(total_rows, HEADS, HEAD_DIM).astype(jnp.float32)
    values_split = value_rows.reshape(total_rows, HEADS, HEAD_DIM).astype(jnp.float32)
    bias_split = jnp.transpose(key_bias.astype(jnp.float32))
    score_scale = HEAD_DIM ** (-0.5)

    def one_shard(shard_pair):
        shard_query, shard_index = shard_pair
        query_pos = shard_index * TOK_A + jnp.arange(TOK_A, dtype=jnp.int32)
        own_block = shard_index * TOK_A // block_rows

        def backward_turn(turn_index, carried_pair):
            output, carried = carried_pair
            block_start = ((own_block - turn_index) * block_rows).astype(jnp.int32)
            block_keys = lax.dynamic_slice_in_dim(keys_split, block_start, block_rows, 0)
            block_values = lax.dynamic_slice_in_dim(values_split, block_start, block_rows, 0)
            block_bias = lax.dynamic_slice_in_dim(bias_split, block_start, block_rows, 1)
            scores = jnp.einsum('qhd,khd->hqk', shard_query, block_keys) * score_scale + block_bias[:, None, :]
            key_pos = block_start + jnp.arange(block_rows, dtype=jnp.int32)
            causal = (key_pos[None, :] < query_pos[:, None])[None]
            fail_logs = jnp.where(causal, -jax.nn.softplus(scores), 0.0)
            later_sum = lax.cumsum(fail_logs, axis=2, reverse=True) - fail_logs + carried[:, :, None]
            weights = jnp.where(causal, jnp.exp(jax.nn.log_sigmoid(scores) + later_sum), 0.0)
            weights = lax.optimization_barrier(weights.astype(jnp.bfloat16)).astype(jnp.float32)
            output = output + jnp.einsum('hqk,khd->qhd', weights, block_values)
            return (output, carried + lax.optimization_barrier(jnp.sum(fail_logs, axis=2)))
        zero_output = jnp.zeros((TOK_A, HEADS, HEAD_DIM), jnp.float32)
        zero_carried = jnp.zeros((HEADS, TOK_A), jnp.float32)
        output, unused = lax.fori_loop(0, own_block + 1, backward_turn, (zero_output, zero_carried))
        return output
    outputs = lax.map(one_shard, (query_split, jnp.arange(N_EP, dtype=jnp.int32)))
    return outputs.reshape(total_rows, HEADS * HEAD_DIM).astype(jnp.bfloat16)

def grouped_product(left_rows, right_matrix):
    part_width = left_rows.shape[1] // N_TP
    summed = jnp.zeros((left_rows.shape[0], right_matrix.shape[1]), jnp.float32)
    for part_index in range(N_TP):
        lower = part_index * part_width
        piece_sum = jnp.dot(left_rows[:, lower:lower + part_width], right_matrix[lower:lower + part_width], preferred_element_type=jnp.float32).astype(jnp.bfloat16)
        summed = summed + lax.optimization_barrier(piece_sum).astype(jnp.float32)
    return summed

def swiglu(chosen_rows, gate_weight, up_weight):
    gate_part = jnp.dot(chosen_rows, gate_weight, preferred_element_type=jnp.float32)
    up_part = jnp.dot(chosen_rows, up_weight, preferred_element_type=jnp.float32)
    return (jax.nn.silu(gate_part) * up_part).astype(jnp.bfloat16)

def routed_experts(normed, expert_index, route_weights, expert_gate, expert_up, expert_down):
    token_count = normed.shape[0]
    flat_expert = expert_index.reshape(-1).astype(jnp.int32)
    flat_token = jnp.repeat(jnp.arange(token_count, dtype=jnp.int32), TOPK)
    flat_weight = route_weights.reshape(-1)
    sort_order = jnp.argsort(flat_expert, stable=True)
    window = token_count // ROWS_B * CAP
    sorted_token = jnp.concatenate([flat_token[sort_order], jnp.zeros((window,), jnp.int32)])
    sorted_weight = jnp.concatenate([flat_weight[sort_order], jnp.zeros((window,), flat_weight.dtype)])
    counts = jax.ops.segment_sum(jnp.ones_like(flat_expert), flat_expert, EXPERTS).astype(jnp.int32)
    starts = (jnp.cumsum(counts) - counts).astype(jnp.int32)

    def one_expert(routed, expert_number):
        first_slot = starts[expert_number]
        tokens = lax.dynamic_slice_in_dim(sorted_token, first_slot, window)
        weights = lax.dynamic_slice_in_dim(sorted_weight, first_slot, window)
        live_slots = jnp.arange(window, dtype=jnp.int32) < counts[expert_number]
        chosen_rows = normed[tokens]
        hidden = swiglu(chosen_rows, expert_gate[expert_number], expert_up[expert_number])
        output = grouped_product(hidden, expert_down[expert_number]).astype(jnp.bfloat16)
        output = lax.optimization_barrier(output).astype(jnp.float32)
        return (routed.at[tokens].add(jnp.where(live_slots, weights, 0.0)[:, None] * output), None)
    routed, unused = lax.scan(one_expert, jnp.zeros((token_count, D), jnp.float32), jnp.arange(EXPERTS, dtype=jnp.int32))
    return routed

def reference(query_rows, key_rows, value_rows, key_bias, mixer_weight, mixer_gain, routed_input, entry_gain, expert_index, route_weights, expert_gate, expert_up, expert_down, shared_gate, shared_up, shared_down, exit_gain):
    attended = stick_breaking(query_rows, key_rows, value_rows, key_bias)
    mixer_sum = grouped_product(attended, mixer_weight)
    mixer_out = root_norm(mixer_sum, mixer_gain).astype(jnp.bfloat16)
    normed = root_norm(routed_input.astype(jnp.float32), entry_gain).astype(jnp.bfloat16)
    routed = routed_experts(normed, expert_index, route_weights, expert_gate, expert_up, expert_down)
    shared_hidden = swiglu(normed, shared_gate, shared_up)
    shared = grouped_product(shared_hidden, shared_down)
    expert_out = root_norm(routed + shared, exit_gain).astype(jnp.bfloat16)
    return (mixer_out, expert_out)
```

```python
import jax
import jax.numpy as jnp
from jax import lax
from jax.experimental import pallas as pl
from jax.experimental.pallas import tpu as pltpu
from jax.sharding import PartitionSpec as P

EPS = 1e-06
TILE = 128


def root_norm(values, gain_row):
    return values * lax.rsqrt(jnp.mean(values * values, axis=-1, keepdims=True) + EPS) * gain_row


def attention_kernel(slot_ref, query_ref, gathered_ref, out_ref, tri_ref, carry_ref):
    head_size = out_ref.shape[1] // 2
    tiles = query_ref.shape[0] // TILE
    ranks = gathered_ref.shape[0]
    keys = 2 * TILE
    slot = slot_ref[0]
    stride = ranks // 2
    row = lax.broadcasted_iota(jnp.int32, (keys, keys), 0)
    col = lax.broadcasted_iota(jnp.int32, (keys, keys), 1)
    tri_ref[...] = (row > col).astype(jnp.float32).astype(jnp.bfloat16)
    out_ref[...] = jnp.zeros(out_ref.shape, jnp.float32)
    carry_ref[...] = jnp.zeros(carry_ref.shape, jnp.float32)

    def pair(place, active, masked_tile):
        first = (2 * place) % ranks
        group = place // stride
        start = pl.multiple_of(group * TILE, TILE)
        pair_rows = jnp.concatenate(
            [gathered_ref[first, pl.ds(start, TILE), :], gathered_ref[first + 1, pl.ds(start, TILE), :]], axis=0
        )
        line = lax.broadcasted_iota(jnp.int32, (16, TILE), 0) == group
        base = tiles * TILE
        bias = jnp.concatenate(
            [
                jnp.sum(
                    jnp.where(line, gathered_ref[first + side, base : base + 16, :].astype(jnp.float32), 0.0),
                    axis=0,
                    keepdims=True,
                )
                for side in (0, 1)
            ],
            axis=1,
        )
        tri = tri_ref[...]
        for tile in active:
            rows = slice(tile * TILE, (tile + 1) * TILE)
            scores = lax.dot_general(
                query_ref[rows, :], pair_rows, (((1,), (1,)), ((), ())), preferred_element_type=jnp.float32
            )
            scores = scores + bias
            log_term = jnp.log(1.0 + jnp.exp(-jnp.abs(scores)))
            fails = jnp.maximum(scores, 0.0) + log_term
            if tile == masked_tile:
                query_at = lax.broadcasted_iota(jnp.int32, (TILE, keys), 0) + (slot % 2) * TILE
                causal = lax.broadcasted_iota(jnp.int32, (TILE, keys), 1) < query_at
                fails = jnp.where(causal, fails, 0.0)
            high = fails.astype(jnp.bfloat16)
            low = (fails - high.astype(jnp.float32)).astype(jnp.bfloat16)
            later = jnp.dot(high, tri, preferred_element_type=jnp.float32)
            later = later + jnp.dot(low, tri, preferred_element_type=jnp.float32)
            carry = carry_ref[rows, 0:1]
            weights = jnp.exp(jnp.minimum(scores, 0.0) - log_term - (later + carry))
            if tile == masked_tile:
                weights = jnp.where(causal, weights, 0.0)
            out_ref[rows, :] += jnp.dot(weights.astype(jnp.bfloat16), pair_rows, preferred_element_type=jnp.float32)
            carry_ref[rows, 0:1] = carry + later[:, 0:1] + fails[:, 0:1]

    half = slot // 2
    for segment in reversed(range(tiles)):
        active = range(segment, tiles)
        top = segment * stride + half
        pair(top, active, segment)
        count = half if segment == 0 else stride - 1

        def turn(index, _, top=top, active=active):
            pair(top - 1 - index, active, None)
            return 0

        lax.fori_loop(0, count, turn, 0)


def attend(slot, queries, gathered):
    tiles = queries.shape[0] // TILE
    return pl.pallas_call(
        attention_kernel,
        grid_spec=pltpu.PrefetchScalarGridSpec(
            num_scalar_prefetch=1,
            grid=(1,),
            in_specs=[
                pl.BlockSpec(queries.shape, lambda i, s: (0, 0)),
                pl.BlockSpec(gathered.shape, lambda i, s: (0, 0, 0)),
            ],
            out_specs=pl.BlockSpec((tiles * TILE, TILE), lambda i, s: (0, 0)),
            scratch_shapes=[
                pltpu.VMEM((2 * TILE, 2 * TILE), jnp.bfloat16),
                pltpu.VMEM((tiles * TILE, TILE), jnp.float32),
            ],
        ),
        out_shape=jax.ShapeDtypeStruct((tiles * TILE, TILE), jnp.float32),
        name="attend",
    )(slot.reshape(1).astype(jnp.int32), queries, gathered)


def expert_kernel(*refs, sizes):
    count = len(sizes)
    rows_in = refs[:count]
    gate_ref, up_ref, down_ref = refs[count : count + 3]
    rows_out = refs[count + 3 : 2 * count + 3]
    stack_ref = refs[2 * count + 3]
    lead = (0,) * (len(gate_ref.shape) - 2)
    start = 0
    for ref, size in zip(rows_in, sizes):
        stack_ref[start : start + size, :] = ref[...]
        start += size
    gate = jnp.dot(stack_ref[...], gate_ref[lead], preferred_element_type=jnp.float32)
    up = jnp.dot(stack_ref[...], up_ref[lead], preferred_element_type=jnp.float32)
    hidden = (gate / (1.0 + jnp.exp(-gate)) * up).astype(jnp.bfloat16)
    start = 0
    for ref, size in zip(rows_out, sizes):
        ref[...] = jnp.dot(
            hidden[start : start + size], down_ref[lead], preferred_element_type=jnp.float32
        ).astype(jnp.bfloat16)
        start += size


def expert_layer(pieces, gate, up, down, which=None):
    sizes = tuple(piece.shape[0] for piece in pieces)
    width = pieces[0].shape[1]

    def whole(shape):
        return pl.BlockSpec(shape, lambda i: (0,) * len(shape))

    def chosen(weight):
        if which is None:
            return whole(weight.shape)
        return pl.BlockSpec((1,) + weight.shape[1:], lambda i: (which, 0, 0))

    return pl.pallas_call(
        lambda *refs: expert_kernel(*refs, sizes=sizes),
        grid=(1,),
        in_specs=[whole(piece.shape) for piece in pieces] + [chosen(gate), chosen(up), chosen(down)],
        out_specs=[whole(piece.shape) for piece in pieces],
        out_shape=[jax.ShapeDtypeStruct(piece.shape, jnp.bfloat16) for piece in pieces],
        scratch_shapes=[pltpu.VMEM((sum(sizes), width), jnp.bfloat16)],
        name="expert_layer",
    )(*pieces, gate, up, down)


def shift(array, by):
    peers = lax.axis_size("tp")
    return lax.ppermute(array, "tp", [(i, (i + by) % peers) for i in range(peers)])


def ring_gather(rows):
    half = rows.shape[0] // 2
    low, high = rows[:half], rows[half:]
    prev_low = shift(low, 1)
    next_high = shift(high, -1)
    prev_high = shift(high, 1)
    next_low = shift(low, -1)
    far_low = shift(prev_low, 1)
    far_high = shift(next_high, -1)
    return (rows, prev_low, prev_high, next_low, next_high, far_low, far_high)


def added(first, second):
    return (first.astype(jnp.float32) + second.astype(jnp.float32)).astype(jnp.bfloat16)


def ring_reduce(parts):
    own, prev_low, prev_high, next_low, next_high, far_low, far_high = parts
    from_low = shift(far_low, -1)
    from_high = shift(far_high, 1)
    back_high = shift(prev_high, -1)
    back_low = shift(next_low, 1)
    down_low = shift(added(prev_low, from_low), -1)
    up_high = shift(added(next_high, from_high), 1)
    half = own.shape[0] // 2
    f32 = jnp.float32
    low = own[:half].astype(f32) + down_low.astype(f32) + back_low.astype(f32)
    high = own[half:].astype(f32) + back_high.astype(f32) + up_high.astype(f32)
    return jnp.concatenate([low, high], axis=0)


def on_device(
    query_rows,
    key_rows,
    value_rows,
    key_bias,
    mixer_weight,
    mixer_gain,
    routed_input,
    entry_gain,
    expert_index,
    route_weights,
    expert_gate,
    expert_up,
    expert_down,
    shared_gate,
    shared_up,
    shared_down,
    exit_gain,
):
    bf16, f32 = jnp.bfloat16, jnp.float32
    shard_rows = query_rows.shape[0]
    head_count = key_bias.shape[1]
    head_size = query_rows.shape[1] // head_count
    ep_size = lax.axis_size("ep")
    ranks = ep_size // head_count
    own_index = lax.axis_index("ep")
    same_rank = [[rank + ranks * head for head in range(head_count)] for rank in range(ranks)]
    same_head = [[head * ranks + rank for rank in range(ranks)] for head in range(head_count)]

    row_count = routed_input.shape[0]
    top_count = expert_index.shape[1]
    local_experts = expert_gate.shape[0]
    model_width = routed_input.shape[1]
    expert_count = local_experts * ep_size
    capacity = 3 * row_count * top_count // (2 * expert_count)
    slot_total = expert_count * capacity
    chunk_slots = ep_size * capacity

    normed = root_norm(routed_input.astype(f32), entry_gain).astype(bf16)
    flat_expert = expert_index.reshape(-1)
    onehot = (flat_expert[:, None] == jnp.arange(expert_count, dtype=jnp.int32)[None, :]).astype(jnp.int32)
    slot_rank = jnp.sum((jnp.cumsum(onehot, axis=0) - onehot) * onehot, axis=1)
    slot_index = (
        (flat_expert % local_experts) * chunk_slots + (flat_expert // local_experts) * capacity + slot_rank
    ).reshape(row_count, top_count)
    matches = slot_index[None, :, :] == jnp.arange(slot_total, dtype=jnp.int32)[:, None, None]
    selector = jnp.any(matches, axis=2).astype(bf16)
    outgoing = jnp.dot(selector, normed, preferred_element_type=f32).astype(bf16)
    arrived = [
        lax.all_to_all(
            outgoing[k * chunk_slots : (k + 1) * chunk_slots].reshape(ep_size, capacity, model_width),
            "ep",
            split_axis=0,
            concat_axis=0,
            tiled=True,
        ).reshape(chunk_slots, model_width)
        for k in range(local_experts)
    ]

    by_head = lambda rows: jnp.transpose(rows.reshape(shard_rows, head_count, head_size), (1, 0, 2))
    query_part = jnp.pad(by_head(query_rows * bf16(head_size ** (-0.5))), ((0, 0), (0, 0), (0, head_size)))
    key_value = jnp.concatenate([by_head(key_rows), by_head(value_rows)], axis=2)
    bias_part = jnp.pad(jnp.transpose(key_bias)[:, None, :], ((0, 0), (0, 15), (0, 0)))
    packed = jnp.concatenate([query_part, key_value, bias_part], axis=1)
    swapped = lax.all_to_all(packed, "ep", 0, 0, axis_index_groups=same_rank, tiled=True)
    queries = swapped[:, :shard_rows].reshape(head_count * shard_rows, 2 * head_size)
    bias_rows = jnp.pad(swapped[:, 2 * shard_rows], ((0, 16 - head_count), (0, 0)))
    sending = jnp.concatenate(
        [swapped[:, shard_rows : 2 * shard_rows].reshape(head_count * shard_rows, 2 * head_size), bias_rows], axis=0
    )
    gathered = lax.all_gather(sending, "ep", axis=0, axis_index_groups=same_head)

    shared_parts = expert_layer(ring_gather(normed), shared_gate, shared_up, shared_down)

    returned = []
    for k in range(local_experts):
        parts = expert_layer(ring_gather(arrived[k]), expert_gate, expert_up, expert_down, which=k)
        rows = ring_reduce(parts).astype(bf16).reshape(ep_size, capacity, model_width)
        back = lax.all_to_all(rows, "ep", split_axis=0, concat_axis=0, tiled=True)
        returned.append(back.reshape(chunk_slots, model_width))

    output = attend(own_index % ranks, queries, gathered)
    per_tile = output[:, head_size:].astype(bf16).reshape(head_count, shard_rows, head_size)
    heads_back = lax.all_to_all(per_tile, "ep", 0, 0, axis_index_groups=same_rank, tiled=True)
    attended = jnp.transpose(heads_back, (1, 0, 2)).reshape(shard_rows, head_count * head_size)
    mixer_term = jnp.dot(attended, mixer_weight, preferred_element_type=f32).astype(bf16)
    mixer_tiles = lax.all_to_all(
        mixer_term.reshape(lax.axis_size("tp"), -1, model_width), "tp", 0, 0, tiled=True
    )
    mixer_sum = jnp.sum(mixer_tiles.astype(f32), axis=0)
    mixer_out = root_norm(mixer_sum, mixer_gain).astype(bf16)

    shared_sum = ring_reduce(shared_parts)
    weighted = jnp.sum(
        jnp.where(
            slot_index[:, :, None] == jnp.arange(slot_total, dtype=jnp.int32)[None, None, :],
            route_weights[:, :, None],
            0.0,
        ),
        axis=1,
    )
    high = weighted.astype(bf16)
    low = (weighted - high.astype(f32)).astype(bf16)
    combined = shared_sum
    for k in range(local_experts):
        lanes = slice(k * chunk_slots, (k + 1) * chunk_slots)
        combined = combined + jnp.dot(high[:, lanes], returned[k], preferred_element_type=f32)
        combined = combined + jnp.dot(low[:, lanes], returned[k], preferred_element_type=f32)
    expert_out = root_norm(combined, exit_gain).astype(bf16)
    return (mixer_out, expert_out)


def solution(mesh):
    in_specs = (
        P("ep", "tp"),
        P("ep", "tp"),
        P("ep", "tp"),
        P("ep", "tp"),
        P("tp", None),
        P(),
        P(("ep", "tp"), None),
        P(),
        P(("ep", "tp"), None),
        P(("ep", "tp"), None),
        P("ep", None, "tp"),
        P("ep", None, "tp"),
        P("ep", "tp", None),
        P(None, "tp"),
        P(None, "tp"),
        P("tp", None),
        P(),
    )
    out_specs = (P(("ep", "tp"), None), P(("ep", "tp"), None))
    return jax.shard_map(
        on_device, mesh=mesh, in_specs=in_specs, out_specs=out_specs, check_vma=False
    )
```

```python
import jax
import jax.numpy as jnp
from jax import lax
from jax.experimental import pallas as pl
from jax.experimental.pallas import tpu as pltpu
from jax.sharding import PartitionSpec as P

EPS = 1e-06
TILE = 128
LANES = 128
TOGETHER = (1, 2, 2, 4)


def root_norm(values, gain_row):
    return values * lax.rsqrt(jnp.mean(values * values, axis=-1, keepdims=True) + EPS) * gain_row


def attention_kernel(slot_ref, query_ref, *refs):
    out_ref, gathered_ref, tri_ref, carry_ref = refs[-4:]
    tiles = query_ref.shape[0] // TILE
    stride = gathered_ref.shape[1]
    keys = 2 * TILE
    slot = slot_ref[0]
    for piece in range(4):
        gathered_ref[slot % 2, 2 * piece : 2 * piece + 2] = refs[piece][...]
        gathered_ref[1 - slot % 2, 2 * piece : 2 * piece + 2] = refs[4 + piece][...]
    row = lax.broadcasted_iota(jnp.int32, (keys, keys), 0)
    col = lax.broadcasted_iota(jnp.int32, (keys, keys), 1)
    tri_ref[...] = (row > col).astype(jnp.float32).astype(jnp.bfloat16)
    out_ref[...] = jnp.zeros(out_ref.shape, jnp.float32)
    carry_ref[...] = jnp.zeros(carry_ref.shape, jnp.float32)

    def pair(place, active, masked_tile):
        group = place // stride
        behind = place % 4 - (slot // 2) % 4
        block = 2 * jnp.where(behind < 0, behind + 4, behind) + (place % stride // 4 + slot // stride) % 2
        start = pl.multiple_of(group * TILE, TILE)
        pair_rows = jnp.concatenate(
            [gathered_ref[side, block, pl.ds(start, TILE), :] for side in (0, 1)], axis=0
        )
        line = lax.broadcasted_iota(jnp.int32, (16, TILE), 0) == group
        base = tiles * TILE
        bias = jnp.concatenate(
            [
                jnp.sum(
                    jnp.where(line, gathered_ref[side, block, base : base + 16, :].astype(jnp.float32), 0.0),
                    axis=0,
                    keepdims=True,
                )
                for side in (0, 1)
            ],
            axis=1,
        )
        rows = slice(active[0] * TILE, tiles * TILE)
        height = (tiles - active[0]) * TILE
        scores = lax.dot_general(
            query_ref[rows, :], pair_rows, (((1,), (1,)), ((), ())), preferred_element_type=jnp.float32
        )
        scores = scores + bias
        log_term = jnp.log(1.0 + jnp.exp(-jnp.abs(scores)))
        fails = jnp.maximum(scores, 0.0) + log_term
        if masked_tile is not None:
            query_at = lax.broadcasted_iota(jnp.int32, (height, keys), 0)
            query_at = jnp.where(query_at < TILE, query_at + (slot % 2) * TILE, keys)
            causal = lax.broadcasted_iota(jnp.int32, (height, keys), 1) < query_at
            fails = jnp.where(causal, fails, 0.0)
        later = jnp.dot(fails.astype(jnp.bfloat16), tri_ref[...], preferred_element_type=jnp.float32)
        carry = carry_ref[rows, 0:1]
        weights = jnp.exp(jnp.minimum(scores, 0.0) - log_term - (later + carry))
        if masked_tile is not None:
            weights = jnp.where(causal, weights, 0.0)
        out_ref[rows, :] += jnp.dot(weights.astype(jnp.bfloat16), pair_rows, preferred_element_type=jnp.float32)
        carry_ref[rows, 0:1] = carry + jnp.sum(fails, axis=1, keepdims=True)

    half = slot // 2
    for segment in reversed(range(tiles)):
        active = range(segment, tiles)
        top = segment * stride + half
        if segment == 0:
            pair(top, active, segment)

            def last(index, _):
                pair(half - 1 - index, active, None)
                return 0

            lax.fori_loop(0, half, last, 0)
            continue
        together = TOGETHER[segment]
        for turn in range(together):
            pair(top - turn, active, segment if turn == 0 else None)

        def turns(index, _, top=top, active=active, together=together):
            for turn in range(together):
                pair(top - (index + 1) * together - turn, active, None)
            return 0

        lax.fori_loop(0, stride // together - 1, turns, 0)


def attend(slot, queries, mine, other):
    tiles = queries.shape[0] // TILE
    return pl.pallas_call(
        attention_kernel,
        grid_spec=pltpu.PrefetchScalarGridSpec(
            num_scalar_prefetch=1,
            grid=(1,),
            in_specs=[
                pl.BlockSpec(queries.shape, lambda i, s: (0, 0)),
            ]
            + [pl.BlockSpec(mine[0].shape, lambda i, s: (0, 0, 0))] * 8,
            out_specs=pl.BlockSpec((tiles * TILE, TILE), lambda i, s: (0, 0)),
            scratch_shapes=[
                pltpu.VMEM((2, 8) + mine[0].shape[1:], jnp.bfloat16),
                pltpu.VMEM((2 * TILE, 2 * TILE), jnp.bfloat16),
                pltpu.VMEM((tiles * TILE, TILE), jnp.float32),
            ],
        ),
        out_shape=jax.ShapeDtypeStruct((tiles * TILE, TILE), jnp.float32),
        name="attend",
    )(slot.reshape(1).astype(jnp.int32), queries, *mine, *other)


def pack_kernel(query_ref, key_ref, value_ref, bias_ref, out_ref):
    f32 = jnp.float32
    rows, heads = bias_ref.shape
    size = query_ref.shape[1] // heads
    bias = jnp.concatenate([bias_ref[...].astype(f32), jnp.zeros((rows, TILE - heads), f32)], axis=1).T
    line = lax.broadcasted_iota(jnp.int32, (16, TILE), 0)
    for head in range(heads):
        lanes = slice(head * size, (head + 1) * size)
        query = query_ref[:, lanes].astype(f32) * size ** (-0.5)
        out_ref[head, :rows, :] = jnp.concatenate([query, jnp.zeros((rows, size), f32)], axis=1).astype(jnp.bfloat16)
        both = jnp.concatenate([key_ref[:, lanes].astype(f32), value_ref[:, lanes].astype(f32)], axis=1)
        out_ref[head, rows : 2 * rows, :] = both.astype(jnp.bfloat16)
        out_ref[head, 2 * rows :, :] = jnp.where(line == 0, bias[head : head + 1, :], 0.0).astype(jnp.bfloat16)


def pack(query_rows, key_rows, value_rows, key_bias):
    rows, heads = key_bias.shape
    return pl.pallas_call(
        pack_kernel,
        out_shape=jax.ShapeDtypeStruct((heads, 2 * rows + 16, TILE), jnp.bfloat16),
        name="pack",
    )(query_rows, key_rows, value_rows, key_bias)


def swiglu(gate, up):
    return gate / (1.0 + jnp.exp(-gate)) * up


def expert_kernel(*refs, sizes):
    count = len(sizes)
    f32, bf16 = jnp.float32, jnp.bfloat16
    rows_in = refs[:count]
    gate_ref, up_ref, down_ref, shared_gate_ref, shared_up_ref, shared_down_ref = refs[count : count + 6]
    rows_out = refs[count + 6 : 2 * count + 6]
    stack_ref = refs[2 * count + 6]
    width = stack_ref.shape[1] - LANES
    start = 0
    for ref, size in zip(rows_in, sizes):
        stack_ref[start : start + size, :] = ref[...]
        start += size
    notes = stack_ref[:, width:].astype(f32)
    weight = notes[:, 0:1] + notes[:, 1:2]
    chosen = notes[:, 2:3]
    rows = stack_ref[:, :width]
    routed = swiglu(
        jnp.dot(rows, gate_ref[0], preferred_element_type=f32), jnp.dot(rows, up_ref[0], preferred_element_type=f32)
    )
    routed = (routed * weight).astype(bf16)
    shared = swiglu(
        jnp.dot(rows, shared_gate_ref[...], preferred_element_type=f32),
        jnp.dot(rows, shared_up_ref[...], preferred_element_type=f32),
    )
    shared = (shared * chosen).astype(bf16)
    start = 0
    for ref, size in zip(rows_out, sizes):
        part = slice(start, start + size)
        ref[...] = (
            jnp.dot(routed[part], down_ref[0], preferred_element_type=f32)
            + jnp.dot(shared[part], shared_down_ref[...], preferred_element_type=f32)
        ).astype(bf16)
        start += size


def expert_layer(pieces, expert, shared, which):
    sizes = tuple(piece.shape[0] for piece in pieces)
    full = pieces[0].shape[1]
    width = full - LANES
    return pl.pallas_call(
        lambda *refs: expert_kernel(*refs, sizes=sizes),
        grid=(1,),
        in_specs=[pl.BlockSpec(piece.shape, lambda i: (0, 0)) for piece in pieces]
        + [pl.BlockSpec((1,) + weight.shape[1:], lambda i: (which, 0, 0)) for weight in expert]
        + [pl.BlockSpec(weight.shape, lambda i: (0, 0)) for weight in shared],
        out_specs=[pl.BlockSpec((size, width), lambda i: (0, 0)) for size in sizes],
        out_shape=[jax.ShapeDtypeStruct((size, width), jnp.bfloat16) for size in sizes],
        scratch_shapes=[pltpu.VMEM((sum(sizes), full), jnp.bfloat16)],
        name="expert_layer",
    )(*pieces, *expert, *shared)


def shift(array, by):
    peers = lax.axis_size("tp")
    return lax.ppermute(array, "tp", [(i, (i + by) % peers) for i in range(peers)])


def ring_gather(low, high):
    prev_low = shift(low, 1)
    next_high = shift(high, -1)
    prev_high = shift(high, 1)
    next_low = shift(low, -1)
    far_low = shift(prev_low, 1)
    far_high = shift(next_high, -1)
    return (low, high, prev_low, prev_high, next_low, next_high, far_low, far_high)


def added(first, second):
    return (first.astype(jnp.float32) + second.astype(jnp.float32)).astype(jnp.bfloat16)


def ring_reduce(parts):
    own_low, own_high, prev_low, prev_high, next_low, next_high, far_low, far_high = parts
    from_low = shift(far_low, -1)
    from_high = shift(far_high, 1)
    back_high = shift(prev_high, -1)
    back_low = shift(next_low, 1)
    down_low = shift(added(prev_low, from_low), -1)
    up_high = shift(added(next_high, from_high), 1)
    f32 = jnp.float32
    low = own_low.astype(f32) + down_low.astype(f32) + back_low.astype(f32)
    high = own_high.astype(f32) + back_high.astype(f32) + up_high.astype(f32)
    return jnp.concatenate([low, high], axis=0)


def after(array, *others):
    return lax.optimization_barrier((array, *others))[0]


def on_device(
    query_rows,
    key_rows,
    value_rows,
    key_bias,
    mixer_weight,
    mixer_gain,
    routed_input,
    entry_gain,
    expert_index,
    route_weights,
    expert_gate,
    expert_up,
    expert_down,
    shared_gate,
    shared_up,
    shared_down,
    exit_gain,
):
    bf16, f32 = jnp.bfloat16, jnp.float32
    shard_rows = query_rows.shape[0]
    head_count = key_bias.shape[1]
    head_size = query_rows.shape[1] // head_count
    ep_size = lax.axis_size("ep")
    ranks = ep_size // head_count
    own_index = lax.axis_index("ep")
    same_rank = [[rank + ranks * head for head in range(head_count)] for rank in range(ranks)]

    row_count = routed_input.shape[0]
    top_count = expert_index.shape[1]
    local_experts = expert_gate.shape[0]
    model_width = routed_input.shape[1]
    expert_count = local_experts * ep_size
    capacity = 3 * row_count * top_count // (2 * expert_count)
    slot_total = expert_count * capacity
    chunk_slots = ep_size * capacity

    normed = root_norm(routed_input.astype(f32), entry_gain).astype(bf16)
    flat_expert = expert_index.reshape(-1)
    places = jnp.arange(row_count * top_count, dtype=jnp.int32)
    earlier = (flat_expert[:, None] == flat_expert[None, :]) & (places[None, :] < places[:, None])
    slot_rank = jnp.sum(earlier.astype(jnp.int32), axis=1)
    slot_index = (
        (flat_expert // local_experts) * local_experts * capacity + (flat_expert % local_experts) * capacity + slot_rank
    )
    selector = (slot_index[None, :] == jnp.arange(slot_total, dtype=jnp.int32)[:, None]).astype(bf16)
    flat_weight = route_weights.reshape(-1)
    weight_high = flat_weight.astype(bf16)
    weight_low = (flat_weight - weight_high.astype(f32)).astype(bf16)
    chosen = (places % top_count == 0).astype(bf16)
    notes = jnp.pad(jnp.stack([weight_high, weight_low, chosen], axis=1), ((0, 0), (0, LANES - 3)))
    any_choice = jnp.sum(selector.reshape(slot_total, row_count, top_count), axis=2)
    outgoing = jnp.concatenate(
        [
            jnp.dot(any_choice, normed, preferred_element_type=f32).astype(bf16),
            jnp.dot(selector, notes, preferred_element_type=f32).astype(bf16),
        ],
        axis=1,
    )

    def exchange(rows):
        return lax.all_to_all(rows, "ep", split_axis=0, concat_axis=0, tiled=True)

    packed = pack(query_rows, key_rows, value_rows, key_bias)
    swapped = lax.all_to_all(packed, "ep", 0, 0, axis_index_groups=same_rank, tiled=True)
    queries = swapped[:, :shard_rows].reshape(head_count * shard_rows, 2 * head_size)
    bias_rows = jnp.pad(swapped[:, 2 * shard_rows], ((0, 16 - head_count), (0, 0)))
    sending = jnp.concatenate(
        [swapped[:, shard_rows : 2 * shard_rows].reshape(head_count * shard_rows, 2 * head_size), bias_rows], axis=0
    )

    def moved(array, target):
        return lax.ppermute(array, "ep", [(i, target(i)) for i in range(ep_size)])

    def around(by):
        return lambda i: i - i % 8 + (i % 8 + 2 * by) % 8

    beside = moved(sending, lambda i: i ^ (ranks // 2))
    near = jnp.stack([sending, beside])
    prev = moved(near, around(1))
    following = moved(near, around(-1))
    across = moved(near, around(2))
    mine = (near, following, across, prev)
    other = tuple(moved(piece, lambda i: i ^ 1) for piece in mine)

    output = attend(own_index % ranks, queries, mine, other)
    outgoing = after(outgoing, sending)
    arrived = exchange(outgoing.reshape(ep_size, local_experts * capacity, model_width + LANES))
    arrived = after(arrived, output)
    half = ep_size // 2
    arrived = [
        tuple(
            arrived[side * half : (side + 1) * half, k * capacity : (k + 1) * capacity].reshape(
                half * capacity, model_width + LANES
            )
            for side in (0, 1)
        )
        for k in range(local_experts)
    ]

    expert = (expert_gate, expert_up, expert_down)
    shared = (shared_gate, shared_up, shared_down)
    gathered_rows = []
    for block in arrived:
        gathered_rows.append(ring_gather(*block))
    returned = []
    for k in range(local_experts):
        parts = expert_layer(gathered_rows[k], expert, shared, k)
        rows = ring_reduce(parts).astype(bf16).reshape(ep_size, capacity, model_width)
        returned.append(exchange(rows).reshape(chunk_slots, model_width))

    per_tile = output[:, head_size:].astype(bf16).reshape(head_count, shard_rows, head_size)
    heads_back = lax.all_to_all(per_tile, "ep", 0, 0, axis_index_groups=same_rank, tiled=True)
    attended = jnp.transpose(heads_back, (1, 0, 2)).reshape(shard_rows, head_count * head_size)
    mixer_term = jnp.dot(attended, mixer_weight, preferred_element_type=f32).astype(bf16)
    mixer_tiles = lax.all_to_all(
        mixer_term.reshape(lax.axis_size("tp"), -1, model_width), "tp", 0, 0, tiled=True
    )
    mixer_sum = jnp.sum(mixer_tiles.astype(f32), axis=0)
    mixer_out = root_norm(mixer_sum, mixer_gain).astype(bf16)

    homes = any_choice.reshape(ep_size, local_experts, capacity, row_count)
    combined = sum(
        lax.dot_general(
            homes[:, k].reshape(chunk_slots, row_count),
            returned[k],
            (((0,), (0,)), ((), ())),
            preferred_element_type=f32,
        )
        for k in range(local_experts)
    )
    expert_out = root_norm(combined, exit_gain).astype(bf16)
    return (mixer_out, expert_out)


def solution(mesh):
    in_specs = (
        P("ep", "tp"),
        P("ep", "tp"),
        P("ep", "tp"),
        P("ep", "tp"),
        P("tp", None),
        P(),
        P(("ep", "tp"), None),
        P(),
        P(("ep", "tp"), None),
        P(("ep", "tp"), None),
        P("ep", None, "tp"),
        P("ep", None, "tp"),
        P("ep", "tp", None),
        P(None, "tp"),
        P(None, "tp"),
        P("tp", None),
        P(),
    )
    out_specs = (P(("ep", "tp"), None), P(("ep", "tp"), None))


    return jax.shard_map(on_device, mesh=mesh, in_specs=in_specs, out_specs=out_specs, check_vma=False)
```

```python
import jax
import jax.numpy as jnp
from jax import lax
from jax.experimental import pallas as pl
from jax.experimental.pallas import tpu as pltpu
from jax.sharding import PartitionSpec as P

EPS = 1e-06
TILE = 128
LANES = 128
TOGETHER = (1, 1, 2, 4)


def root_norm(values, gain_row):
    return values * lax.rsqrt(jnp.mean(values * values, axis=-1, keepdims=True) + EPS) * gain_row


def attention_kernel(slot_ref, query_ref, *refs):
    out_ref, gathered_ref, tri_ref, carry_ref = refs[-4:]
    tiles = query_ref.shape[0] // TILE
    stride = gathered_ref.shape[1]
    keys = 2 * TILE
    slot = slot_ref[0]
    for piece in range(4):
        gathered_ref[slot % 2, 2 * piece : 2 * piece + 2] = refs[piece][...]
        gathered_ref[1 - slot % 2, 2 * piece : 2 * piece + 2] = refs[4 + piece][...]
    row = lax.broadcasted_iota(jnp.int32, (keys, keys), 0)
    col = lax.broadcasted_iota(jnp.int32, (keys, keys), 1)
    tri_ref[...] = (row > col).astype(jnp.float32).astype(jnp.bfloat16)
    out_ref[...] = jnp.zeros(out_ref.shape, jnp.float32)
    carry_ref[...] = jnp.zeros(carry_ref.shape, jnp.float32)

    def pair(place, active, masked_tile):
        group = place // stride
        behind = place % 4 - (slot // 2) % 4
        block = 2 * jnp.where(behind < 0, behind + 4, behind) + (place % stride // 4 + slot // stride) % 2
        start = pl.multiple_of(group * TILE, TILE)
        pair_rows = jnp.concatenate(
            [gathered_ref[side, block, pl.ds(start, TILE), :] for side in (0, 1)], axis=0
        )
        line = lax.broadcasted_iota(jnp.int32, (16, TILE), 0) == group
        base = tiles * TILE
        bias = jnp.concatenate(
            [
                jnp.sum(
                    jnp.where(line, gathered_ref[side, block, base : base + 16, :].astype(jnp.float32), 0.0),
                    axis=0,
                    keepdims=True,
                )
                for side in (0, 1)
            ],
            axis=1,
        )
        rows = slice(active[0] * TILE, tiles * TILE)
        height = (tiles - active[0]) * TILE
        scores = lax.dot_general(
            query_ref[rows, :], pair_rows, (((1,), (1,)), ((), ())), preferred_element_type=jnp.float32
        )
        scores = scores + bias
        log_term = jnp.log(1.0 + jnp.exp(-jnp.abs(scores)))
        fails = jnp.maximum(scores, 0.0) + log_term
        if masked_tile is not None:
            query_at = lax.broadcasted_iota(jnp.int32, (height, keys), 0)
            query_at = jnp.where(query_at < TILE, query_at + (slot % 2) * TILE, keys)
            causal = lax.broadcasted_iota(jnp.int32, (height, keys), 1) < query_at
            fails = jnp.where(causal, fails, 0.0)
        later = jnp.dot(fails.astype(jnp.bfloat16), tri_ref[...], preferred_element_type=jnp.float32)
        carry = carry_ref[rows, 0:1]
        weights = jnp.exp(jnp.minimum(scores, 0.0) - log_term - (later + carry))
        if masked_tile is not None:
            weights = jnp.where(causal, weights, 0.0)
        out_ref[rows, :] += jnp.dot(weights.astype(jnp.bfloat16), pair_rows, preferred_element_type=jnp.float32)
        carry_ref[rows, 0:1] = carry + jnp.sum(fails, axis=1, keepdims=True)

    half = slot // 2
    for segment in reversed(range(tiles)):
        active = range(segment, tiles)
        top = segment * stride + half
        if segment == 0:
            pair(top, active, segment)

            def last(index, _):
                pair(half - 1 - index, active, None)
                return 0

            lax.fori_loop(0, half, last, 0)
            continue
        together = TOGETHER[segment]
        for turn in range(together):
            pair(top - turn, active, segment if turn == 0 else None)

        def turns(index, _, top=top, active=active, together=together):
            for turn in range(together):
                pair(top - (index + 1) * together - turn, active, None)
            return 0

        lax.fori_loop(0, stride // together - 1, turns, 0)


def attend(slot, queries, mine, other):
    tiles = queries.shape[0] // TILE
    return pl.pallas_call(
        attention_kernel,
        grid_spec=pltpu.PrefetchScalarGridSpec(
            num_scalar_prefetch=1,
            grid=(1,),
            in_specs=[
                pl.BlockSpec(queries.shape, lambda i, s: (0, 0)),
            ]
            + [pl.BlockSpec(mine[0].shape, lambda i, s: (0, 0, 0))] * 8,
            out_specs=pl.BlockSpec((tiles * TILE, TILE), lambda i, s: (0, 0)),
            scratch_shapes=[
                pltpu.VMEM((2, 8) + mine[0].shape[1:], jnp.bfloat16),
                pltpu.VMEM((2 * TILE, 2 * TILE), jnp.bfloat16),
                pltpu.VMEM((tiles * TILE, TILE), jnp.float32),
            ],
        ),
        out_shape=jax.ShapeDtypeStruct((tiles * TILE, TILE), jnp.float32),
        name="attend",
    )(slot.reshape(1).astype(jnp.int32), queries, *mine, *other)


def pack_kernel(query_ref, key_ref, value_ref, bias_ref, out_ref):
    f32 = jnp.float32
    rows, heads = bias_ref.shape
    size = query_ref.shape[1] // heads
    bias = jnp.concatenate([bias_ref[...].astype(f32), jnp.zeros((rows, TILE - heads), f32)], axis=1).T
    line = lax.broadcasted_iota(jnp.int32, (16, TILE), 0)
    for head in range(heads):
        lanes = slice(head * size, (head + 1) * size)
        query = query_ref[:, lanes].astype(f32) * size ** (-0.5)
        out_ref[head, :rows, :] = jnp.concatenate([query, jnp.zeros((rows, size), f32)], axis=1).astype(jnp.bfloat16)
        both = jnp.concatenate([key_ref[:, lanes].astype(f32), value_ref[:, lanes].astype(f32)], axis=1)
        out_ref[head, rows : 2 * rows, :] = both.astype(jnp.bfloat16)
        out_ref[head, 2 * rows :, :] = jnp.where(line == 0, bias[head : head + 1, :], 0.0).astype(jnp.bfloat16)


def pack(query_rows, key_rows, value_rows, key_bias):
    rows, heads = key_bias.shape
    return pl.pallas_call(
        pack_kernel,
        out_shape=jax.ShapeDtypeStruct((heads, 2 * rows + 16, TILE), jnp.bfloat16),
        name="pack",
    )(query_rows, key_rows, value_rows, key_bias)


def swiglu(gate, up):
    return gate / (1.0 + jnp.exp(-gate)) * up


def expert_kernel(*refs, sizes):
    count = len(sizes)
    f32, bf16 = jnp.float32, jnp.bfloat16
    rows_in = refs[:count]
    gate_ref, up_ref, down_ref, shared_gate_ref, shared_up_ref, shared_down_ref = refs[count : count + 6]
    rows_out = refs[count + 6 : 2 * count + 6]
    stack_ref = refs[2 * count + 6]
    width = stack_ref.shape[1] - LANES
    start = 0
    for ref, size in zip(rows_in, sizes):
        stack_ref[start : start + size, :] = ref[...]
        start += size
    notes = stack_ref[:, width:].astype(f32)
    weight = notes[:, 0:1] + notes[:, 1:2]
    chosen = notes[:, 2:3]
    rows = stack_ref[:, :width]
    routed = swiglu(
        jnp.dot(rows, gate_ref[0], preferred_element_type=f32), jnp.dot(rows, up_ref[0], preferred_element_type=f32)
    )
    routed = (routed * weight).astype(bf16)
    shared = swiglu(
        jnp.dot(rows, shared_gate_ref[...], preferred_element_type=f32),
        jnp.dot(rows, shared_up_ref[...], preferred_element_type=f32),
    )
    shared = (shared * chosen).astype(bf16)
    tile = shared_down_ref.shape[1] // 8
    for column in range(8):
        lanes = slice(column * tile, (column + 1) * tile)
        result = jnp.dot(routed, down_ref[0, :, lanes], preferred_element_type=f32)
        result = result + jnp.dot(shared, shared_down_ref[:, lanes], preferred_element_type=f32)
        result = result.astype(bf16)
        start = 0
        for ref, size in zip(rows_out, sizes):
            ref[:, lanes] = result[start : start + size]
            start += size


def expert_layer(pieces, expert, shared, which):
    sizes = tuple(piece.shape[0] for piece in pieces)
    full = pieces[0].shape[1]
    width = full - LANES
    return pl.pallas_call(
        lambda *refs: expert_kernel(*refs, sizes=sizes),
        grid=(1,),
        in_specs=[pl.BlockSpec(piece.shape, lambda i: (0, 0)) for piece in pieces]
        + [pl.BlockSpec((1,) + weight.shape[1:], lambda i: (which, 0, 0)) for weight in expert]
        + [pl.BlockSpec(weight.shape, lambda i: (0, 0)) for weight in shared],
        out_specs=[pl.BlockSpec((size, width), lambda i: (0, 0)) for size in sizes],
        out_shape=[jax.ShapeDtypeStruct((size, width), jnp.bfloat16) for size in sizes],
        scratch_shapes=[pltpu.VMEM((sum(sizes), full), jnp.bfloat16)],
        name="expert_layer",
    )(*pieces, *expert, *shared)


def shift(array, by):
    peers = lax.axis_size("tp")
    return lax.ppermute(array, "tp", [(i, (i + by) % peers) for i in range(peers)])


def ring_gather(low, high):
    prev_low = shift(low, 1)
    next_high = shift(high, -1)
    prev_high = shift(high, 1)
    next_low = shift(low, -1)
    far_low = shift(prev_low, 1)
    far_high = shift(next_high, -1)
    return (low, high, prev_low, prev_high, next_low, next_high, far_low, far_high)


def added(first, second):
    return (first.astype(jnp.float32) + second.astype(jnp.float32)).astype(jnp.bfloat16)


def ring_reduce(parts):
    own_low, own_high, prev_low, prev_high, next_low, next_high, far_low, far_high = parts
    back_high = shift(prev_high, -1)
    back_low = shift(next_low, 1)
    from_low = shift(far_low, -1)
    from_high = shift(far_high, 1)
    down_low = shift(added(prev_low, from_low), -1)
    up_high = shift(added(next_high, from_high), 1)
    f32 = jnp.float32
    low = own_low.astype(f32) + down_low.astype(f32) + back_low.astype(f32)
    high = own_high.astype(f32) + back_high.astype(f32) + up_high.astype(f32)
    return (low.astype(jnp.bfloat16), high.astype(jnp.bfloat16))


def after(array, *others):
    return lax.optimization_barrier((array, *others))[0]


def on_device(
    query_rows,
    key_rows,
    value_rows,
    key_bias,
    mixer_weight,
    mixer_gain,
    routed_input,
    entry_gain,
    expert_index,
    route_weights,
    expert_gate,
    expert_up,
    expert_down,
    shared_gate,
    shared_up,
    shared_down,
    exit_gain,
):
    bf16, f32 = jnp.bfloat16, jnp.float32
    shard_rows = query_rows.shape[0]
    head_count = key_bias.shape[1]
    head_size = query_rows.shape[1] // head_count
    ep_size = lax.axis_size("ep")
    ranks = ep_size // head_count
    own_index = lax.axis_index("ep")
    same_rank = [[rank + ranks * head for head in range(head_count)] for rank in range(ranks)]

    row_count = routed_input.shape[0]
    top_count = expert_index.shape[1]
    local_experts = expert_gate.shape[0]
    model_width = routed_input.shape[1]
    expert_count = local_experts * ep_size
    capacity = 3 * row_count * top_count // (2 * expert_count)
    slot_total = expert_count * capacity
    chunk_slots = ep_size * capacity

    normed = root_norm(routed_input.astype(f32), entry_gain).astype(bf16)
    flat_expert = expert_index.reshape(-1)
    places = jnp.arange(row_count * top_count, dtype=jnp.int32)
    earlier = (flat_expert[:, None] == flat_expert[None, :]) & (places[None, :] < places[:, None])
    slot_rank = jnp.sum(earlier.astype(jnp.int32), axis=1)
    slot_index = (
        (flat_expert // local_experts) * local_experts * capacity + (flat_expert % local_experts) * capacity + slot_rank
    )
    selector = (slot_index[None, :] == jnp.arange(slot_total, dtype=jnp.int32)[:, None]).astype(bf16)
    flat_weight = route_weights.reshape(-1)
    weight_high = flat_weight.astype(bf16)
    weight_low = (flat_weight - weight_high.astype(f32)).astype(bf16)
    chosen = (places % top_count == 0).astype(bf16)
    notes = jnp.pad(jnp.stack([weight_high, weight_low, chosen], axis=1), ((0, 0), (0, LANES - 3)))
    any_choice = jnp.sum(selector.reshape(slot_total, row_count, top_count), axis=2)
    outgoing = jnp.concatenate(
        [
            jnp.dot(any_choice, normed, preferred_element_type=f32).astype(bf16),
            jnp.dot(selector, notes, preferred_element_type=f32).astype(bf16),
        ],
        axis=1,
    )

    def exchange(rows):
        return lax.all_to_all(rows, "ep", split_axis=0, concat_axis=0, tiled=True)

    packed = pack(query_rows, key_rows, value_rows, key_bias)
    swapped = lax.all_to_all(packed, "ep", 0, 0, axis_index_groups=same_rank, tiled=True)
    queries = swapped[:, :shard_rows].reshape(head_count * shard_rows, 2 * head_size)
    bias_rows = jnp.pad(swapped[:, 2 * shard_rows], ((0, 16 - head_count), (0, 0)))
    sending = jnp.concatenate(
        [swapped[:, shard_rows : 2 * shard_rows].reshape(head_count * shard_rows, 2 * head_size), bias_rows], axis=0
    )

    def moved(array, target):
        return lax.ppermute(array, "ep", [(i, target(i)) for i in range(ep_size)])

    def around(by):
        return lambda i: i - i % 8 + (i % 8 + 2 * by) % 8

    beside = moved(sending, lambda i: i ^ (ranks // 2))
    near = jnp.stack([sending, beside])
    prev = moved(near, around(1))
    following = moved(near, around(-1))
    across = moved(near, around(2))
    mine = (near, following, across, prev)
    other = tuple(moved(piece, lambda i: i ^ 1) for piece in mine)

    output = attend(own_index % ranks, queries, mine, other)
    outgoing = after(outgoing, sending)
    arrived = exchange(outgoing.reshape(ep_size, local_experts * capacity, model_width + LANES))
    arrived = after(arrived, output)
    low, high = (
        arrived[:, k * capacity : (k + 1) * capacity].reshape(chunk_slots, model_width + LANES)
        for k in range(local_experts)
    )

    expert = (expert_gate, expert_up, expert_down)
    shared = (shared_gate, shared_up, shared_down)
    low, high, prev_low, prev_high, next_low, next_high, far_low, far_high = ring_gather(low, high)
    own_low, prev_low, next_low = expert_layer((low, prev_low, next_low), expert, shared, 0)
    own_high, prev_high, next_high = expert_layer((high, prev_high, next_high), expert, shared, 1)
    (far_low,) = expert_layer((far_low,), expert, shared, 0)
    (far_high,) = expert_layer((far_high,), expert, shared, 1)
    low, high = ring_reduce((own_low, own_high, prev_low, prev_high, next_low, next_high, far_low, far_high))
    rows = jnp.concatenate([part.reshape(ep_size, capacity, model_width) for part in (low, high)], axis=1)
    returned = exchange(rows).reshape(slot_total, model_width)

    per_tile = output[:, head_size:].astype(bf16).reshape(head_count, shard_rows, head_size)
    heads_back = lax.all_to_all(per_tile, "ep", 0, 0, axis_index_groups=same_rank, tiled=True)
    attended = jnp.transpose(heads_back, (1, 0, 2)).reshape(shard_rows, head_count * head_size)
    mixer_term = jnp.dot(attended, mixer_weight, preferred_element_type=f32).astype(bf16)
    mixer_tiles = lax.all_to_all(
        mixer_term.reshape(lax.axis_size("tp"), -1, model_width), "tp", 0, 0, tiled=True
    )
    mixer_sum = jnp.sum(mixer_tiles.astype(f32), axis=0)
    mixer_out = root_norm(mixer_sum, mixer_gain).astype(bf16)

    combined = lax.dot_general(any_choice, returned, (((0,), (0,)), ((), ())), preferred_element_type=f32)
    expert_out = root_norm(combined, exit_gain).astype(bf16)
    return (mixer_out, expert_out)


def solution(mesh):
    in_specs = (
        P("ep", "tp"),
        P("ep", "tp"),
        P("ep", "tp"),
        P("ep", "tp"),
        P("tp", None),
        P(),
        P(("ep", "tp"), None),
        P(),
        P(("ep", "tp"), None),
        P(("ep", "tp"), None),
        P("ep", None, "tp"),
        P("ep", None, "tp"),
        P("ep", "tp", None),
        P(None, "tp"),
        P(None, "tp"),
        P("tp", None),
        P(),
    )
    out_specs = (P(("ep", "tp"), None), P(("ep", "tp"), None))


    return jax.shard_map(on_device, mesh=mesh, in_specs=in_specs, out_specs=out_specs, check_vma=False)
```

```python
import jax
import jax.numpy as jnp
from jax import lax
from jax.experimental import pallas as pl
from jax.experimental.pallas import tpu as pltpu
from jax.sharding import PartitionSpec as P

EPS = 1e-06
TILE = 128
LANES = 128
TOGETHER = (1, 1, 2, 4)


def root_norm(values, gain_row):
    return values * lax.rsqrt(jnp.mean(values * values, axis=-1, keepdims=True) + EPS) * gain_row


def attention_kernel(slot_ref, query_ref, *refs):
    out_ref, gathered_ref, tri_ref, carry_ref = refs[-4:]
    tiles = query_ref.shape[0] // TILE
    stride = gathered_ref.shape[1]
    keys = 2 * TILE
    slot = slot_ref[0]
    for piece in range(4):
        gathered_ref[slot % 2, 2 * piece : 2 * piece + 2] = refs[piece][...]
        gathered_ref[1 - slot % 2, 2 * piece : 2 * piece + 2] = refs[4 + piece][...]
    row = lax.broadcasted_iota(jnp.int32, (keys, keys), 0)
    col = lax.broadcasted_iota(jnp.int32, (keys, keys), 1)
    tri_ref[...] = (row > col).astype(jnp.float32).astype(jnp.bfloat16)
    out_ref[...] = jnp.zeros(out_ref.shape, jnp.float32)
    carry_ref[...] = jnp.zeros(carry_ref.shape, jnp.float32)

    def pair(place, active, masked_tile):
        group = place // stride
        behind = place % 4 - (slot // 2) % 4
        block = 2 * jnp.where(behind < 0, behind + 4, behind) + (place % stride // 4 + slot // stride) % 2
        start = pl.multiple_of(group * TILE, TILE)
        pair_rows = jnp.concatenate(
            [gathered_ref[side, block, pl.ds(start, TILE), :] for side in (0, 1)], axis=0
        )
        line = lax.broadcasted_iota(jnp.int32, (16, TILE), 0) == group
        base = tiles * TILE
        bias = jnp.concatenate(
            [
                jnp.sum(
                    jnp.where(line, gathered_ref[side, block, base : base + 16, :].astype(jnp.float32), 0.0),
                    axis=0,
                    keepdims=True,
                )
                for side in (0, 1)
            ],
            axis=1,
        )
        rows = slice(active[0] * TILE, tiles * TILE)
        height = (tiles - active[0]) * TILE
        scores = lax.dot_general(
            query_ref[rows, :], pair_rows, (((1,), (1,)), ((), ())), preferred_element_type=jnp.float32
        )
        scores = scores + bias
        log_term = jnp.log(1.0 + jnp.exp(-jnp.abs(scores)))
        fails = jnp.maximum(scores, 0.0) + log_term
        if masked_tile is not None:
            query_at = lax.broadcasted_iota(jnp.int32, (height, keys), 0)
            query_at = jnp.where(query_at < TILE, query_at + (slot % 2) * TILE, keys)
            causal = lax.broadcasted_iota(jnp.int32, (height, keys), 1) < query_at
            fails = jnp.where(causal, fails, 0.0)
        later = jnp.dot(fails.astype(jnp.bfloat16), tri_ref[...], preferred_element_type=jnp.float32)
        carry = carry_ref[rows, 0:1]
        weights = jnp.exp(jnp.minimum(scores, 0.0) - log_term - (later + carry))
        if masked_tile is not None:
            weights = jnp.where(causal, weights, 0.0)
        out_ref[rows, :] += jnp.dot(weights.astype(jnp.bfloat16), pair_rows, preferred_element_type=jnp.float32)
        carry_ref[rows, 0:1] = carry + jnp.sum(fails, axis=1, keepdims=True)

    half = slot // 2
    for segment in reversed(range(tiles)):
        active = range(segment, tiles)
        top = segment * stride + half
        if segment == 0:
            pair(top, active, segment)

            def last(index, _):
                pair(half - 1 - index, active, None)
                return 0

            lax.fori_loop(0, half, last, 0)
            continue
        together = TOGETHER[segment]
        for turn in range(together):
            pair(top - turn, active, segment if turn == 0 else None)

        def turns(index, _, top=top, active=active, together=together):
            for turn in range(together):
                pair(top - (index + 1) * together - turn, active, None)
            return 0

        lax.fori_loop(0, stride // together - 1, turns, 0)


def attend(slot, queries, mine, other):
    tiles = queries.shape[0] // TILE
    return pl.pallas_call(
        attention_kernel,
        grid_spec=pltpu.PrefetchScalarGridSpec(
            num_scalar_prefetch=1,
            grid=(1,),
            in_specs=[
                pl.BlockSpec(queries.shape, lambda i, s: (0, 0)),
            ]
            + [pl.BlockSpec(mine[0].shape, lambda i, s: (0, 0, 0))] * 8,
            out_specs=pl.BlockSpec((tiles * TILE, TILE), lambda i, s: (0, 0)),
            scratch_shapes=[
                pltpu.VMEM((2, 8) + mine[0].shape[1:], jnp.bfloat16),
                pltpu.VMEM((2 * TILE, 2 * TILE), jnp.bfloat16),
                pltpu.VMEM((tiles * TILE, TILE), jnp.float32),
            ],
        ),
        out_shape=jax.ShapeDtypeStruct((tiles * TILE, TILE), jnp.float32),
        name="attend",
    )(slot.reshape(1).astype(jnp.int32), queries, *mine, *other)


def pack_kernel(query_ref, key_ref, value_ref, bias_ref, out_ref):
    f32 = jnp.float32
    heads, rows = bias_ref.shape
    size = query_ref.shape[1] // heads
    bias = bias_ref[...].astype(f32)
    line = lax.broadcasted_iota(jnp.int32, (16, TILE), 0)
    for head in range(heads):
        lanes = slice(head * size, (head + 1) * size)
        query = query_ref[:, lanes].astype(f32) * size ** (-0.5)
        out_ref[head, :rows, :] = jnp.concatenate([query, jnp.zeros((rows, size), f32)], axis=1).astype(jnp.bfloat16)
        both = jnp.concatenate([key_ref[:, lanes].astype(f32), value_ref[:, lanes].astype(f32)], axis=1)
        out_ref[head, rows : 2 * rows, :] = both.astype(jnp.bfloat16)
        out_ref[head, 2 * rows :, :] = jnp.where(line == 0, bias[head : head + 1, :], 0.0).astype(jnp.bfloat16)


def pack(query_rows, key_rows, value_rows, key_bias):
    rows, heads = key_bias.shape
    return pl.pallas_call(
        pack_kernel,
        out_shape=jax.ShapeDtypeStruct((heads, 2 * rows + 16, TILE), jnp.bfloat16),
        name="pack",
    )(query_rows, key_rows, value_rows, jnp.transpose(key_bias))


def swiglu(gate, up):
    return gate / (1.0 + jnp.exp(-gate)) * up


def expert_kernel(*refs, sizes):
    count = len(sizes)
    f32, bf16 = jnp.float32, jnp.bfloat16
    rows_in = refs[:count]
    gate_ref, up_ref, down_ref, shared_gate_ref, shared_up_ref, shared_down_ref = refs[count : count + 6]
    rows_out = refs[count + 6 : 2 * count + 6]
    stack_ref = refs[2 * count + 6]
    width = stack_ref.shape[1] - LANES
    start = 0
    for ref, size in zip(rows_in, sizes):
        stack_ref[start : start + size, :] = ref[...]
        start += size
    notes = stack_ref[:, width:].astype(f32)
    weight = notes[:, 0:1] + notes[:, 1:2]
    chosen = notes[:, 2:3]
    rows = stack_ref[:, :width]
    routed = swiglu(
        jnp.dot(rows, gate_ref[0], preferred_element_type=f32), jnp.dot(rows, up_ref[0], preferred_element_type=f32)
    )
    routed = (routed * weight).astype(bf16)
    shared = swiglu(
        jnp.dot(rows, shared_gate_ref[...], preferred_element_type=f32),
        jnp.dot(rows, shared_up_ref[...], preferred_element_type=f32),
    )
    shared = (shared * chosen).astype(bf16)
    tile = shared_down_ref.shape[1] // 8
    for column in range(8):
        lanes = slice(column * tile, (column + 1) * tile)
        result = jnp.dot(routed, down_ref[0, :, lanes], preferred_element_type=f32)
        result = result + jnp.dot(shared, shared_down_ref[:, lanes], preferred_element_type=f32)
        result = result.astype(bf16)
        start = 0
        for ref, size in zip(rows_out, sizes):
            ref[:, lanes] = result[start : start + size]
            start += size


def expert_layer(pieces, expert, shared, which):
    sizes = tuple(piece.shape[0] for piece in pieces)
    full = pieces[0].shape[1]
    width = full - LANES
    return pl.pallas_call(
        lambda *refs: expert_kernel(*refs, sizes=sizes),
        grid=(1,),
        in_specs=[pl.BlockSpec(piece.shape, lambda i: (0, 0)) for piece in pieces]
        + [pl.BlockSpec((1,) + weight.shape[1:], lambda i: (which, 0, 0)) for weight in expert]
        + [pl.BlockSpec(weight.shape, lambda i: (0, 0)) for weight in shared],
        out_specs=[pl.BlockSpec((size, width), lambda i: (0, 0)) for size in sizes],
        out_shape=[jax.ShapeDtypeStruct((size, width), jnp.bfloat16) for size in sizes],
        scratch_shapes=[pltpu.VMEM((sum(sizes), full), jnp.bfloat16)],
        name="expert_layer",
    )(*pieces, *expert, *shared)


def shift(array, by):
    peers = lax.axis_size("tp")
    return lax.ppermute(array, "tp", [(i, (i + by) % peers) for i in range(peers)])


def ring_gather(low, high):
    prev_low = shift(low, 1)
    next_high = shift(high, -1)
    prev_high = shift(high, 1)
    next_low = shift(low, -1)
    far_low = shift(prev_low, 1)
    far_high = shift(next_high, -1)
    return (low, high, prev_low, prev_high, next_low, next_high, far_low, far_high)


def added(first, second):
    return (first.astype(jnp.float32) + second.astype(jnp.float32)).astype(jnp.bfloat16)


def ring_reduce(parts):
    own_low, own_high, prev_low, prev_high, next_low, next_high, far_low, far_high = parts
    back_high = shift(prev_high, -1)
    back_low = shift(next_low, 1)
    from_low = shift(far_low, -1)
    from_high = shift(far_high, 1)
    down_low = shift(added(prev_low, from_low), -1)
    up_high = shift(added(next_high, from_high), 1)
    f32 = jnp.float32
    low = own_low.astype(f32) + down_low.astype(f32) + back_low.astype(f32)
    high = own_high.astype(f32) + back_high.astype(f32) + up_high.astype(f32)
    return (low.astype(jnp.bfloat16), high.astype(jnp.bfloat16))


def after(array, *others):
    return lax.optimization_barrier((array, *others))[0]


def on_device(
    query_rows,
    key_rows,
    value_rows,
    key_bias,
    mixer_weight,
    mixer_gain,
    routed_input,
    entry_gain,
    expert_index,
    route_weights,
    expert_gate,
    expert_up,
    expert_down,
    shared_gate,
    shared_up,
    shared_down,
    exit_gain,
):
    bf16, f32 = jnp.bfloat16, jnp.float32
    shard_rows = query_rows.shape[0]
    head_count = key_bias.shape[1]
    head_size = query_rows.shape[1] // head_count
    ep_size = lax.axis_size("ep")
    ranks = ep_size // head_count
    own_index = lax.axis_index("ep")
    same_rank = [[rank + ranks * head for head in range(head_count)] for rank in range(ranks)]

    row_count = routed_input.shape[0]
    top_count = expert_index.shape[1]
    local_experts = expert_gate.shape[0]
    model_width = routed_input.shape[1]
    expert_count = local_experts * ep_size
    capacity = 3 * row_count * top_count // (2 * expert_count)
    slot_total = expert_count * capacity
    chunk_slots = ep_size * capacity

    normed = root_norm(routed_input.astype(f32), entry_gain).astype(bf16)
    flat_expert = jnp.transpose(expert_index).reshape(-1)
    places = jnp.arange(row_count * top_count, dtype=jnp.int32)
    earlier = (flat_expert[:, None] == flat_expert[None, :]) & (places[None, :] < places[:, None])
    slot_rank = jnp.sum(earlier.astype(jnp.int32), axis=1)
    slot_index = (
        (flat_expert // local_experts) * local_experts * capacity + (flat_expert % local_experts) * capacity + slot_rank
    )
    selector = (slot_index[None, :] == jnp.arange(slot_total, dtype=jnp.int32)[:, None]).astype(bf16)
    flat_weight = jnp.transpose(route_weights).reshape(-1)
    weight_high = flat_weight.astype(bf16)
    weight_low = (flat_weight - weight_high.astype(f32)).astype(bf16)
    chosen = (places < row_count).astype(bf16)
    notes = jnp.pad(jnp.stack([weight_high, weight_low, chosen], axis=1), ((0, 0), (0, LANES - 3)))
    any_choice = jnp.sum(selector.reshape(slot_total, top_count, row_count), axis=1)
    outgoing = jnp.concatenate(
        [
            jnp.dot(any_choice, normed, preferred_element_type=f32).astype(bf16),
            jnp.dot(selector, notes, preferred_element_type=f32).astype(bf16),
        ],
        axis=1,
    )

    def exchange(rows):
        return lax.all_to_all(rows, "ep", split_axis=0, concat_axis=0, tiled=True)

    packed = pack(query_rows, key_rows, value_rows, key_bias)
    swapped = lax.all_to_all(packed, "ep", 0, 0, axis_index_groups=same_rank, tiled=True)
    queries = swapped[:, :shard_rows].reshape(head_count * shard_rows, 2 * head_size)
    bias_rows = jnp.pad(swapped[:, 2 * shard_rows], ((0, 16 - head_count), (0, 0)))
    sending = jnp.concatenate(
        [swapped[:, shard_rows : 2 * shard_rows].reshape(head_count * shard_rows, 2 * head_size), bias_rows], axis=0
    )

    def moved(array, target):
        return lax.ppermute(array, "ep", [(i, target(i)) for i in range(ep_size)])

    def around(by):
        return lambda i: i - i % 8 + (i % 8 + 2 * by) % 8

    beside = moved(sending, lambda i: i ^ (ranks // 2))
    near = jnp.stack([sending, beside])
    prev = moved(near, around(1))
    following = moved(near, around(-1))
    across = moved(near, around(2))
    mine = (near, following, across, prev)
    other = tuple(moved(piece, lambda i: i ^ 1) for piece in mine)

    output = attend(own_index % ranks, queries, mine, other)
    outgoing = after(outgoing, sending)
    arrived = exchange(outgoing.reshape(ep_size, local_experts * capacity, model_width + LANES))
    arrived = after(arrived, output)
    low, high = (
        arrived[:, k * capacity : (k + 1) * capacity].reshape(chunk_slots, model_width + LANES)
        for k in range(local_experts)
    )

    expert = (expert_gate, expert_up, expert_down)
    shared = (shared_gate, shared_up, shared_down)
    low, high, prev_low, prev_high, next_low, next_high, far_low, far_high = ring_gather(low, high)
    own_low, prev_low, next_low = expert_layer((low, prev_low, next_low), expert, shared, 0)
    own_high, prev_high, next_high = expert_layer((high, prev_high, next_high), expert, shared, 1)
    (far_low,) = expert_layer((far_low,), expert, shared, 0)
    (far_high,) = expert_layer((far_high,), expert, shared, 1)
    low, high = ring_reduce((own_low, own_high, prev_low, prev_high, next_low, next_high, far_low, far_high))
    rows = jnp.concatenate([part.reshape(ep_size, capacity, model_width) for part in (low, high)], axis=1)
    returned = exchange(rows).reshape(slot_total, model_width)

    per_tile = output[:, head_size:].astype(bf16).reshape(head_count, shard_rows, head_size)
    heads_back = lax.all_to_all(per_tile, "ep", 0, 0, axis_index_groups=same_rank, tiled=True)
    attended = jnp.transpose(heads_back, (1, 0, 2)).reshape(shard_rows, head_count * head_size)
    mixer_term = jnp.dot(attended, mixer_weight, preferred_element_type=f32).astype(bf16)
    mixer_tiles = lax.all_to_all(
        mixer_term.reshape(lax.axis_size("tp"), -1, model_width), "tp", 0, 0, tiled=True
    )
    mixer_sum = jnp.sum(mixer_tiles.astype(f32), axis=0)
    mixer_out = root_norm(mixer_sum, mixer_gain).astype(bf16)

    combined = lax.dot_general(any_choice, returned, (((0,), (0,)), ((), ())), preferred_element_type=f32)
    expert_out = root_norm(combined, exit_gain).astype(bf16)
    return (mixer_out, expert_out)


def solution(mesh):
    in_specs = (
        P("ep", "tp"),
        P("ep", "tp"),
        P("ep", "tp"),
        P("ep", "tp"),
        P("tp", None),
        P(),
        P(("ep", "tp"), None),
        P(),
        P(("ep", "tp"), None),
        P(("ep", "tp"), None),
        P("ep", None, "tp"),
        P("ep", None, "tp"),
        P("ep", "tp", None),
        P(None, "tp"),
        P(None, "tp"),
        P("tp", None),
        P(),
    )
    out_specs = (P(("ep", "tp"), None), P(("ep", "tp"), None))


    return jax.shard_map(on_device, mesh=mesh, in_specs=in_specs, out_specs=out_specs, check_vma=False)
```
